256 devices in a mesh: grp: 2 (over y), sp: 32 (over z, core), tp: 4 (over x).
Axes of the slice: x: 4, y: 2, z: 16, core: 2. Of those that a mesh axis runs over, the one named last changes fastest.
The devices are a block of a 4x16x16 slice.
Arguments:
- residual: bfloat16 [16384, 2048], P(('grp', 'sp')), parts along dimension 0, may hold values from -6 to 6
- queries: bfloat16 [16384, 1024], P(('grp', 'sp'), 'tp'), parts along dimension 0, may hold values from -400 to 400
- keys: bfloat16 [16384, 1024], P(('grp', 'sp'), 'tp'), parts along dimension 0, may hold values from -8 to 8
- values: bfloat16 [16384, 1024], P(('grp', 'sp'), 'tp'), parts along dimension 0, may hold values from -6 to 6
- log_gates: float32 [16384, 16], P(('grp', 'sp'), 'tp'), parts along dimension 0, may hold values from -955 to 0, as said below
- w_out: bfloat16 [1024, 2048], P('tp'), may hold values from -0.75 to 0.75
- norm_gain: float32 [2048], replicated, may hold values from 0.1 to 1.9
- w_gate: bfloat16 [2048, 5632], P('sp', 'tp'), may hold values from -0.125 to 0.125
- w_up: bfloat16 [2048, 5632], P('sp', 'tp'), may hold values from -0.125 to 0.125
- w_down: bfloat16 [5632, 2048], P('tp', 'sp'), may hold values from -0.078125 to 0.078125
Outputs:
- output: bfloat16 [16384, 2048], P(('grp', 'sp', 'tp')), parts along dimension 0
The draws below stay inside these ranges and needn't reach their ends.
There are 2 independent parts, one for each index of `grp`. The reference program is written for one: setup_inputs(seed, part) draws one part's arguments, and reference() takes and returns one part's arrays. A program takes and returns all parts, laid end to end along the dimension named above; an argument that names none is the same for every part. Nothing has to cross between parts.
Inputs may be any that keep to these rules, and one draw needn't show every extreme that they name: `log_gates`: never rises along positions.
All inputs are finite; a program needn't handle non-finite values.
Results may differ from the reference program's by a relative error of at most 0.014.
Values may be sent and summed in bfloat16 or wider, within the bound.
No kernel may reach another device: no remote copies, remote signals or barrier semaphores. Data moves between devices by JAX's collectives and lax.ppermute only.
A program may use at most 128 MiB of HBM per device.

```python
import math
import jax
import jax.numpy as jnp
from jax import lax

D = 2048
ATTN_HEAD_COUNT = 16
HEAD_DIM = 64
FF = 5632
TOK_DEV = 256
SEQUENCE_TOKENS = 8192
N_TP = 4


def layout(key):
    random_seed_key = jax.random.fold_in(key, 31)
    random_ordering_key, random_shift_key, random_back_key, random_stride_key, random_spacing_key, random_strong_key, random_select_key, random_spike_key = jax.random.split(random_seed_key, 8)
    block_count = SEQUENCE_TOKENS // TOK_DEV
    inserted_count = block_count - 2
    quarter = max(TOK_DEV // 4, 1)
    head_order = jax.random.permutation(random_ordering_key, ATTN_HEAD_COUNT)
    gradual_heads = head_order < ATTN_HEAD_COUNT // 2
    block_ids = jnp.arange(inserted_count, dtype=jnp.int32) + 2
    places = block_ids * TOK_DEV + jax.random.randint(random_shift_key, (inserted_count,), 0, quarter)
    matches = (block_ids - 1) * TOK_DEV - 1 - jax.random.randint(random_back_key, (inserted_count,), 0, quarter)
    neighbours = matches - jax.random.randint(random_stride_key, (inserted_count,), 1, 5)
    score_gaps = jax.random.uniform(random_spacing_key, (inserted_count, ATTN_HEAD_COUNT), jnp.float32, 1.0, 2.5)
    strong_decline = jax.random.uniform(random_strong_key, (inserted_count, ATTN_HEAD_COUNT), jnp.float32, math.log(0.02), math.log(0.1))
    picked = jax.random.permutation(random_select_key, inserted_count)[:2]
    sudden_spike = jnp.any(jnp.arange(inserted_count, dtype=jnp.int32)[:, None] == picked[None, :], axis=1)
    sudden_decline = jax.random.uniform(random_spike_key, (inserted_count, ATTN_HEAD_COUNT), jnp.float32, math.log(0.5), math.log(0.8))
    gate_changes = jnp.where(gradual_heads[None, :], jnp.where(sudden_spike[:, None], sudden_decline, 0.0), strong_decline)
    return (gradual_heads, places, matches, neighbours, score_gaps, gate_changes)


def planted(key):
    gradual_heads, places, matches, neighbours, score_gaps, gate_changes = layout(key)
    key_query, key_keys = jax.random.split(jax.random.fold_in(key, 11), 2)
    row_width = ATTN_HEAD_COUNT * HEAD_DIM
    query_rows = jnp.clip(jax.random.normal(key_query, (SEQUENCE_TOKENS, row_width), jnp.float32), -6.0, 6.0)
    key_rows = jnp.clip(jax.random.normal(key_keys, (SEQUENCE_TOKENS, row_width), jnp.float32), -6.0, 6.0)
    inserted_count = places.shape[0]
    levels = jnp.array([8.0, 12.0, 16.0], jnp.float32)
    strength = levels[jnp.arange(inserted_count, dtype=jnp.int32) % 3][:, None, None]
    chosen = key_rows[matches].reshape(inserted_count, ATTN_HEAD_COUNT, HEAD_DIM)
    energy = jnp.maximum(jnp.sum(chosen * chosen, axis=-1, keepdims=True), 0.5 * HEAD_DIM)
    planted_rows = strength * 8.0 * math.sqrt(HEAD_DIM) * chosen / energy
    compensate = (score_gaps + gate_changes)[:, :, None]
    neighbour = chosen * (1.0 - compensate / (8.0 * strength))
    query_rows = jnp.clip(query_rows.at[places].set(planted_rows.reshape(inserted_count, row_width)), -400.0, 400.0)
    key_rows = key_rows.at[neighbours].set(neighbour.reshape(inserted_count, row_width))
    return (query_rows, key_rows)


def draw_queries(key, part):
    return planted(key)[0].astype(jnp.bfloat16)


def draw_keys(key, part):
    return planted(key)[1].astype(jnp.bfloat16)


def draw_log_gates(key, part):
    gradual_heads, places, matches, neighbours, score_gaps, gate_changes = layout(key)
    key_factor, key_jitter = jax.random.split(jax.random.fold_in(key, 23), 2)
    block_count = SEQUENCE_TOKENS // TOK_DEV
    block_factor = jnp.exp(jax.random.uniform(key_factor, (block_count, ATTN_HEAD_COUNT), jnp.float32, math.log(0.5), math.log(2.0)))
    block_factor = jnp.repeat(block_factor, TOK_DEV, axis=0)
    roughness = jax.random.uniform(key_jitter, (SEQUENCE_TOKENS, ATTN_HEAD_COUNT), jnp.float32, 0.5, 1.5)
    head_rates = jnp.where(gradual_heads, 0.5 / SEQUENCE_TOKENS, 1.0 / 40.0)
    forget_logits = -head_rates[None, :] * block_factor * roughness
    clusters = jnp.zeros((SEQUENCE_TOKENS, ATTN_HEAD_COUNT), jnp.float32).at[matches].set(gate_changes)
    return jnp.cumsum(forget_logits + clusters, axis=0)


def shard_levels(key, dims, cuts, least, largest):
    def one(position, shards_of):
        steps = jax.random.uniform(jax.random.fold_in(jax.random.fold_in(key, 6), position), (shards_of,), jnp.float32, least / len(cuts), largest / len(cuts))
        return jnp.repeat(jnp.exp(steps), dims[position] // shards_of).reshape((-1,) + (1,) * (len(dims) - position - 1))

    level = one(*cuts[0])
    for cut in cuts[1:]:
        level = level * one(*cut)
    return level


def gaussian(key, shape, spread, limit, shards=(), kind=jnp.bfloat16):
    loudness = shard_levels(key, shape, shards, -0.22, 0.18) if shards else 1.0
    entries = jax.random.normal(key, shape, jnp.float32) * spread * loudness
    return jnp.minimum(jnp.maximum(entries, -limit), limit).astype(kind)


def setup_inputs(seed: int = 0, part: int = 0) -> dict:
    seeds = jax.random.split(jax.random.key(seed), 11)
    part_splits = jax.random.split(jax.random.fold_in(seeds[10], part), 11)
    return {
        "residual": gaussian(part_splits[0], (SEQUENCE_TOKENS, D), 1.0, 6.0, ((0, 32),)),
        "queries": draw_queries(jax.random.fold_in(jax.random.fold_in(seeds[10], part), 71), part),
        "keys": draw_keys(jax.random.fold_in(jax.random.fold_in(seeds[10], part), 71), part),
        "values": gaussian(part_splits[3], (SEQUENCE_TOKENS, ATTN_HEAD_COUNT * HEAD_DIM), 1.0, 6.0, ((0, 32), (1, 4))),
        "log_gates": draw_log_gates(jax.random.fold_in(jax.random.fold_in(seeds[10], part), 71), part),
        "w_out": gaussian(seeds[5], (ATTN_HEAD_COUNT * HEAD_DIM, D), HEAD_DIM ** -0.5, 0.75, ((0, 4),)),
        "norm_gain": jnp.clip(1.0 + 0.18 * jax.random.normal(seeds[6], (D,), jnp.float32), 0.1, 1.9),
        "w_gate": gaussian(seeds[7], (D, FF), D ** -0.5, 0.125, ((0, 32), (1, 4))),
        "w_up": gaussian(seeds[8], (D, FF), D ** -0.5, 0.125, ((0, 32), (1, 4))),
        "w_down": gaussian(seeds[9], (FF, D), FF ** -0.5, 0.078125, ((0, 4), (1, 32))),
    }


def normalize(rows_in, gain):
    floats = rows_in.astype(jnp.float32)
    scaled = floats * lax.rsqrt(lax.optimization_barrier(jnp.mean(floats * floats, axis=-1, keepdims=True)) + 1e-06)
    return (scaled * gain).astype(jnp.bfloat16)

def group_sum(left, right, groups):
    rows_total = left.shape[0]
    width = left.shape[1] // groups
    left_groups = left.reshape(rows_total, groups, width).astype(jnp.float32)
    right_groups = right.reshape(groups, width, right.shape[1]).astype(jnp.float32)
    partial_terms = jnp.einsum('tgc,gcd->gtd', left_groups, right_groups).astype(jnp.bfloat16)
    partial_terms = lax.optimization_barrier(partial_terms)
    return lax.optimization_barrier(jnp.sum(partial_terms.astype(jnp.float32), axis=0))

def reference(residual, queries, keys, values, log_gates, w_out, norm_gain, w_gate, w_up, w_down):
    score_scale = HEAD_DIM ** (-0.5)
    query_heads = queries.reshape(SEQUENCE_TOKENS, ATTN_HEAD_COUNT, HEAD_DIM)
    key_heads = keys.reshape(SEQUENCE_TOKENS, ATTN_HEAD_COUNT, HEAD_DIM).astype(jnp.float32)
    value_heads = values.reshape(SEQUENCE_TOKENS, ATTN_HEAD_COUNT, HEAD_DIM).astype(jnp.float32)
    block_rows = math.gcd(SEQUENCE_TOKENS, 512)
    key_positions = jnp.arange(SEQUENCE_TOKENS, dtype=jnp.int32)

    def one_block(index_block):
        anchor = (index_block * block_rows).astype(jnp.int32)
        query_block = lax.dynamic_slice_in_dim(query_heads, anchor, block_rows, 0).astype(jnp.float32)
        gate_block = lax.dynamic_slice_in_dim(log_gates, anchor, block_rows, 0)
        scores = jnp.einsum('qhd,khd->hqk', query_block, key_heads) * score_scale
        scores = scores + gate_block.T[:, :, None] - log_gates.T[:, None, :]
        query_positions = anchor + jnp.arange(block_rows, dtype=jnp.int32)
        causal = query_positions[:, None] >= key_positions[None, :]
        scores = jnp.where(causal[None], scores, -jnp.inf)
        row_max = lax.optimization_barrier(jnp.max(scores, axis=-1, keepdims=True))
        weights = jnp.where(causal[None], jnp.exp(scores - row_max), 0.0)
        totals = lax.optimization_barrier(jnp.sum(weights, axis=-1))
        rounded = lax.optimization_barrier(weights.astype(jnp.bfloat16)).astype(jnp.float32)
        summed = jnp.einsum('hqk,khd->hqd', rounded, value_heads) / totals[:, :, None]
        return summed.transpose(1, 0, 2).reshape(block_rows, ATTN_HEAD_COUNT * HEAD_DIM).astype(jnp.bfloat16)
    attended = lax.map(one_block, jnp.arange(SEQUENCE_TOKENS // block_rows, dtype=jnp.int32))
    attended = attended.reshape(SEQUENCE_TOKENS, ATTN_HEAD_COUNT * HEAD_DIM)
    projected = group_sum(attended, w_out, N_TP)
    mixed = (residual.astype(jnp.float32) + projected).astype(jnp.bfloat16)
    normed = normalize(mixed, norm_gain)
    gate_proj = jnp.dot(normed, w_gate, preferred_element_type=jnp.float32)
    up_proj = jnp.dot(normed, w_up, preferred_element_type=jnp.float32)
    hidden = (jax.nn.silu(gate_proj) * up_proj).astype(jnp.bfloat16)
    down_sum = group_sum(hidden, w_down, N_TP)
    summed = mixed.astype(jnp.float32) + 0.5 * down_sum
    scaled = summed * lax.rsqrt(lax.optimization_barrier(jnp.mean(summed * summed, axis=-1, keepdims=True)) + 1e-06)
    return scaled.astype(jnp.bfloat16)
```

```python
import functools

import jax
import jax.numpy as jnp
from jax import lax
from jax.experimental import pallas as pl
from jax.experimental.pallas import tpu as pltpu
from jax.sharding import PartitionSpec as P

GATE_ROWS = 16
MASKED = -1e30


def swap_cores(value):
    n = lax.axis_size("sp")
    return lax.ppermute(value, "sp", [(i, i ^ 1) for i in range(n)])


def chip_shift(value, step):
    n = lax.axis_size("sp")
    return lax.ppermute(value, "sp", [(i, (i + 2 * step) % n) for i in range(n)])


def tp_shift(value, step):
    n = lax.axis_size("tp")
    return lax.ppermute(value, "tp", [(i, (i + step) % n) for i in range(n)])


def swap_groups(value):
    n = lax.axis_size("grp")
    return lax.ppermute(value, "grp", [(i, i ^ 1) for i in range(n)])


def three_parts(value):
    high = lax.reduce_precision(value, 8, 7)
    rest = value - high
    middle = lax.reduce_precision(rest, 8, 7)
    low = rest - middle
    return [p.astype(jnp.bfloat16) for p in (high, middle, low)]


def ring(own, split):
    chips = lax.axis_size("sp") // 2
    up = down = own
    ups, downs = [], []
    for _ in range(1, chips // 2):
        up = chip_shift(up, 1)
        down = chip_shift(down, -1)
        ups.append(up)
        downs.append(down)
    return ups + downs, (chip_shift(up[:split], 1), chip_shift(down[split:], -1))


def attend_kernel(chips, heads, width, tile, place_ref, qa_ref, own_ref, *refs):
    whole = chips - 2
    pieces, (first_ref, second_ref, out_ref, held, top, total, sems) = refs[:whole], refs[whole:]
    place = place_ref[0]
    keys = own_ref.shape[1]
    rows = qa_ref.shape[1]
    key_rows = heads * width
    split = key_rows + GATE_ROWS
    copies = [
        pltpu.make_async_copy(piece, held.at[i], sems.at[i]) for i, piece in enumerate(pieces)
    ]
    copies.append(
        pltpu.make_async_copy(first_ref, held.at[whole, pl.ds(0, split)], sems.at[whole])
    )
    copies.append(
        pltpu.make_async_copy(
            second_ref, held.at[whole, pl.ds(split, keys * key_rows // keys)], sems.at[whole + 1]
        )
    )
    for copy in copies:
        copy.start()
    lane = lax.broadcasted_iota(jnp.int32, (1, key_rows), 1)

    def block(read, opening):
        value_block = jnp.concatenate(
            [read(split, key_rows, j * key_rows, key_rows) for j in range(keys // key_rows)], axis=0
        )
        gate_block = read(key_rows, GATE_ROWS, 0, keys)
        for h in range(heads):
            key_block = jnp.concatenate([read(h * width, width, 0, keys), gate_block], axis=0)
            mine = (lane >= h * width) & (lane < (h + 1) * width)
            values = jnp.where(mine, value_block, jnp.ones_like(value_block))
            for r in range(0, rows, tile):
                at = pl.ds(r, tile)
                scores = jnp.dot(qa_ref[h, at, :], key_block, preferred_element_type=jnp.float32)
                if opening:
                    row = r + lax.broadcasted_iota(jnp.int32, scores.shape, 0)
                    column = lax.broadcasted_iota(jnp.int32, scores.shape, 1)
                    scores = jnp.where(row >= column, scores, MASKED)
                block_top = jnp.max(scores, axis=1, keepdims=True)
                if opening:
                    new_top = block_top
                else:
                    old_top = top[h, at, :1]
                    new_top = jnp.maximum(old_top, block_top)
                weights = jnp.exp(scores - new_top).astype(jnp.bfloat16)
                product = jnp.dot(weights, values, preferred_element_type=jnp.float32)
                if not opening:
                    product += total[h, at, :] * jnp.exp(old_top - new_top)
                total[h, at, :] = product
                top[h, at, :] = jnp.broadcast_to(new_top, (tile, top.shape[2]))

    block(lambda r, m, c, n: own_ref[r : r + m, c : c + n], True)
    for copy in copies:
        copy.wait()

    @pl.loop(0, chips - 1)
    def _(i):
        half = chips // 2
        needed = jnp.where(
            i < half - 1, place - (i + 1), jnp.where(i < whole, place + (i - half + 2) - chips, place - half)
        )

        @pl.when(needed >= 0)
        def _():
            block(lambda r, m, c, n: held[i, r : r + m, c : c + n], False)

    result = jnp.zeros((rows, key_rows), jnp.float32)
    for h in range(heads):
        sums = total[h, :, :]
        mine = (lane >= h * width) & (lane < (h + 1) * width)
        result = jnp.where(mine, sums / pltpu.roll(sums, width, 1), result)
    out_ref[...] = result.astype(out_ref.dtype)


def attend(queries, keys, values, log_gates):
    rows = queries.shape[0]
    heads = log_gates.shape[1] // 2
    columns = queries.shape[1] // 2
    width = columns // heads
    chips = lax.axis_size("sp") // 2
    place = lax.axis_index("sp")
    core = place % 2
    gate_parts = jnp.concatenate(three_parts(log_gates), axis=1)
    gate_parts = gate_parts.reshape(rows, 3, 2, heads)
    sliced = [jnp.moveaxis(gate_parts, 2, 0).reshape(2, rows, 3 * heads)]
    packed = jnp.concatenate([queries, keys, values], axis=1).reshape(rows, 3, 2, columns)
    packed = jnp.moveaxis(packed, 2, 0).reshape(2, rows, 3 * columns)
    padding = jnp.zeros((2, rows, 128 - 3 * heads), jnp.bfloat16)
    packed = jnp.concatenate([packed, sliced[0], padding], axis=2)
    mine = jnp.where(core == 0, packed[0], packed[1])
    theirs = swap_cores(jnp.where(core == 0, packed[1], packed[0]))
    both = jnp.concatenate(
        [jnp.where(core == 0, mine, theirs), jnp.where(core == 0, theirs, mine)], axis=0
    )
    q, k, v = (both[:, i * columns : (i + 1) * columns] for i in range(3))
    gates = both[:, 3 * columns : 3 * columns + 3 * heads].reshape(2 * rows, 3, heads)
    scaled = (q.astype(jnp.float32) * (width**-0.5)).astype(jnp.bfloat16)
    one = jnp.ones((2 * rows, 3), jnp.bfloat16)
    zero = jnp.zeros((2 * rows, 3), jnp.bfloat16)
    augmented = []
    for h in range(heads):
        parts = [scaled[:, h * width : (h + 1) * width], gates[:, :, h]]
        parts += [one if g == h else zero for g in range(heads)]
        parts.append(jnp.zeros((2 * rows, GATE_ROWS - 3 - 3 * heads), jnp.bfloat16))
        augmented.append(jnp.concatenate(parts, axis=1))
    augmented = jnp.stack(augmented)
    gate_rows = jnp.concatenate(
        [one] + [-gates[:, :, h] for h in range(heads)]
        + [jnp.zeros((2 * rows, GATE_ROWS - 3 - 3 * heads), jnp.bfloat16)],
        axis=1,
    ).T
    value_rows = jnp.concatenate(
        [v[r : r + columns] for r in range(0, 2 * rows, columns)], axis=1
    )
    own = jnp.concatenate([k.T, gate_rows, value_rows], axis=0)
    pieces, halves = ring(own, columns + GATE_ROWS)
    return attend_call(chips, heads, width, place // 2, augmented, own, pieces, halves)


def attend_call(chips, heads, width, place, augmented, own, pieces, halves):
    rows = augmented.shape[1]
    anywhere = pl.BlockSpec(memory_space=pl.ANY)
    local = pl.BlockSpec(memory_space=pltpu.VMEM)
    keys = own.shape[1]
    return pl.pallas_call(
        functools.partial(attend_kernel, chips, heads, width, 256),
        out_shape=jax.ShapeDtypeStruct((rows, heads * width), jnp.bfloat16),
        in_specs=[pl.BlockSpec(memory_space=pltpu.SMEM), local, local] + [anywhere] * chips,
        out_specs=local,
        scratch_shapes=[
            pltpu.VMEM((chips - 1, *own.shape), jnp.bfloat16),
            pltpu.VMEM((heads, rows, 128), jnp.float32),
            pltpu.VMEM((heads, rows, heads * width), jnp.float32),
            pltpu.SemaphoreType.DMA((chips,)),
        ],
        compiler_params=pltpu.CompilerParams(vmem_limit_bytes=32 * 2**20),
        cost_estimate=pl.CostEstimate(
            flops=4 * rows * keys * chips * heads * 256,
            bytes_accessed=chips * own.size * 2,
            transcendentals=rows * keys * chips * heads,
        ),
        name="attend",
    )(place.reshape(1), augmented, own, *pieces, *halves)


def in_core_order(mine, theirs, axis):
    core = lax.axis_index("sp") % 2
    first, second = jnp.where(core == 0, mine, theirs), jnp.where(core == 0, theirs, mine)
    return jnp.concatenate([first, second], axis=axis)


def weights_ring(own):
    chips = lax.axis_size("sp") // 2
    half = own.shape[0] // 2
    side = lax.axis_index("grp") % 2
    up = down = jnp.where(side == 0, own[:half], own[half:])
    ups, downs, others = [], [], []
    for _ in range(1, chips // 2):
        up = chip_shift(up, 1)
        down = chip_shift(down, -1)
        ups.append(up)
        downs.append(down)
        others.append(swap_groups(jnp.concatenate([up, down], axis=0)))
    last = [chip_shift(up, 1), chip_shift(others[-1][half:], -1)]
    return [own] + ups + downs + others + last


def project_kernel(groups, cols, place_ref, mine_ref, theirs_ref, *refs):
    weights, (own_ref, other_ref, gain_ref, mixed_ref, normed_ref) = refs[:groups], refs[groups:]
    core = place_ref[0] % 2
    rows, width = mine_ref.shape[0], mine_ref.shape[1] // groups
    half = rows // 2
    features = mixed_ref.shape[1]
    group = []
    for s in range(groups):
        mine = mine_ref[:, s * width : (s + 1) * width]
        theirs = theirs_ref[:, s * width : (s + 1) * width]
        first, second = jnp.where(core == 0, mine, theirs), jnp.where(core == 0, theirs, mine)
        group.append(jnp.concatenate([first, second], axis=1))
    squares = jnp.zeros((rows, 128), jnp.float32)
    for c in range(0, features, cols):
        at = slice(c, c + cols)
        projected = jnp.zeros((rows, cols), jnp.float32)
        for s in range(groups):
            product = jnp.dot(group[s], weights[s][:, at], preferred_element_type=jnp.float32)
            projected += product.astype(jnp.bfloat16).astype(jnp.float32)
        own, other = own_ref[:, at], other_ref[:, at]
        first, second = jnp.where(core == 0, own, other), jnp.where(core == 0, other, own)
        residual = jnp.concatenate([first, second], axis=0).astype(jnp.float32)
        mixed = (residual + projected).astype(jnp.bfloat16)
        mixed_ref[:, at] = mixed
        floats = mixed.astype(jnp.float32)
        for d in range(0, cols, 128):
            squares += floats[:, d : d + 128] * floats[:, d : d + 128]
    scale = lax.rsqrt(jnp.sum(squares, axis=1, keepdims=True) / features + 1e-06)
    for c in range(0, features, cols):
        at = slice(c, c + cols)
        normed = mixed_ref[:, at].astype(jnp.float32) * scale * gain_ref[:, at]
        normed_ref[:, at] = normed.astype(jnp.bfloat16)


def project(mine, theirs, weights, own, other, gain):
    rows, features = 2 * own.shape[0], own.shape[1]
    local = pl.BlockSpec(memory_space=pltpu.VMEM)
    place = lax.axis_index("sp")
    return pl.pallas_call(
        functools.partial(project_kernel, len(weights), 256),
        out_shape=[jax.ShapeDtypeStruct((rows, features), jnp.bfloat16)] * 2,
        in_specs=[pl.BlockSpec(memory_space=pltpu.SMEM)] + [local] * (5 + len(weights)),
        out_specs=[local] * 2,
        compiler_params=pltpu.CompilerParams(vmem_limit_bytes=40 * 2**20),
        cost_estimate=pl.CostEstimate(
            flops=2 * rows * features * 2 * mine.shape[1],
            bytes_accessed=2 * (3 * rows * features + 2 * mine.size),
            transcendentals=rows,
        ),
        name="project",
    )(place.reshape(1), mine, theirs, *weights, own, other, gain.reshape(1, features))


def feed_kernel(chips, cols, where_ref, normed_ref, *refs):
    near = chips // 2 - 1
    pieces, (kept_ref, sent_ref, held, sems) = refs[: 3 + 3 * near], refs[3 + 3 * near :]
    place, side = where_ref[0] // 2, where_ref[1]
    core = where_ref[0] % 2
    half = held.shape[0] // 2
    units = held.shape[0] // 3
    own, ups, downs = pieces[0], pieces[1 : 1 + near], pieces[1 + near : 1 + 2 * near]
    others, last = pieces[1 + 2 * near : 1 + 3 * near], pieces[1 + 3 * near :]

    def spot(chip, part):
        row = pl.multiple_of(part * half, 16)
        column = pl.multiple_of(lax.rem(chip + chips, chips) * 128, 128)
        return held.at[pl.ds(row, half), pl.ds(column, 128)]

    moves = [(own.at[pl.ds(0, half)], spot(place, 0)), (own.at[pl.ds(half, half)], spot(place, 1))]
    for k in range(1, near + 1):
        moves.append((ups[k - 1], spot(place - k, side)))
        moves.append((downs[k - 1], spot(place + k, side)))
        moves.append((others[k - 1].at[pl.ds(0, half)], spot(place - k, 1 - side)))
        moves.append((others[k - 1].at[pl.ds(half, half)], spot(place + k, 1 - side)))
    moves.append((last[0], spot(place + near + 1, side)))
    moves.append((last[1], spot(place + near + 1, 1 - side)))
    copies = [
        pltpu.make_async_copy(source, target, sems.at[i])
        for i, (source, target) in enumerate(moves)
    ]
    for copy in copies:
        copy.start()
    for copy in copies:
        copy.wait()
    contract = (((1,), (1,)), ((), ()))
    gate = lax.dot_general(
        normed_ref[...], held[:units, :], contract, preferred_element_type=jnp.float32
    )
    up = lax.dot_general(
        normed_ref[...], held[units : 2 * units, :], contract, preferred_element_type=jnp.float32
    )
    hidden = (gate / (1.0 + jnp.exp(-gate)) * up).astype(jnp.bfloat16)
    rows = hidden.shape[0] // 2
    for c in range(0, held.shape[1], cols):
        at = slice(c, c + cols)
        partial = jnp.dot(
            hidden, held[2 * units : 3 * units, at], preferred_element_type=jnp.float32
        )
        first, second = partial[:rows], partial[rows:]
        kept_ref[:, at] = jnp.where(core == 0, first, second)
        sent_ref[:, at] = jnp.where(core == 0, second, first).astype(jnp.bfloat16)


def feed(normed, pieces):
    chips = lax.axis_size("sp") // 2
    rows, features = normed.shape
    anywhere = pl.BlockSpec(memory_space=pl.ANY)
    local = pl.BlockSpec(memory_space=pltpu.VMEM)
    where = jnp.stack([lax.axis_index("sp"), lax.axis_index("grp") % 2])
    depth = pieces[0].shape[0]
    return pl.pallas_call(
        functools.partial(feed_kernel, chips, 512),
        out_shape=[
            jax.ShapeDtypeStruct((rows // 2, features), jnp.float32),
            jax.ShapeDtypeStruct((rows // 2, features), jnp.bfloat16),
        ],
        in_specs=[pl.BlockSpec(memory_space=pltpu.SMEM), local] + [anywhere] * len(pieces),
        out_specs=[local] * 2,
        scratch_shapes=[
            pltpu.VMEM((depth, features), jnp.bfloat16),
            pltpu.SemaphoreType.DMA((2 * chips,)),
        ],
        compiler_params=pltpu.CompilerParams(vmem_limit_bytes=48 * 2**20),
        cost_estimate=pl.CostEstimate(
            flops=2 * rows * features * depth,
            bytes_accessed=2 * (depth * features + 2 * rows * features),
            transcendentals=rows * depth // 3,
        ),
        name="feed",
    )(where, normed, *pieces)


def body(residual, queries, keys, values, log_gates, w_out, norm_gain, w_gate, w_up, w_down):
    tp = lax.axis_size("tp")
    core = lax.axis_index("sp") % 2
    units = w_down.shape[0] // 2
    shard = jnp.stack([w_gate.T, w_up.T, w_down]).reshape(3, 2, units, -1)
    shard = jnp.moveaxis(shard, 1, 0).reshape(2, 3 * units, -1)
    mine = jnp.where(core == 0, shard[0], shard[1])
    theirs = swap_cores(jnp.where(core == 0, shard[1], shard[0]))
    pieces = weights_ring(in_core_order(mine, theirs, 1))
    other_residual = swap_cores(residual)
    out_weights = [w_out] + [tp_shift(w_out, s) for s in range(1, tp)]
    attended = attend(queries, keys, values, log_gates)
    groups = [attended] + [tp_shift(attended, s) for s in range(1, tp)]
    mine = jnp.concatenate(groups, axis=1)
    mixed, normed = project(
        mine, swap_cores(mine), out_weights, residual, other_residual, norm_gain
    )
    kept, sent = feed(normed, pieces)
    partial = (kept + swap_cores(sent).astype(jnp.float32)).astype(jnp.bfloat16)
    per_device = partial.shape[0] // tp
    place = lax.axis_index("tp")

    def rows_of(value, index):
        return lax.dynamic_slice_in_dim(value, index * per_device, per_device, 0)

    down_sum = rows_of(partial, place).astype(jnp.float32)
    for s in range(1, tp):
        down_sum += tp_shift(rows_of(partial, (place + s) % tp), s).astype(jnp.float32)
    summed = rows_of(mixed, core * tp + place).astype(jnp.float32) + 0.5 * down_sum
    scaled = summed * lax.rsqrt(jnp.mean(summed * summed, axis=-1, keepdims=True) + 1e-06)
    return scaled.astype(jnp.bfloat16)


def solution(mesh):
    in_specs = (
        P(("grp", "sp"), None),
        P(("grp", "sp"), "tp"),
        P(("grp", "sp"), "tp"),
        P(("grp", "sp"), "tp"),
        P(("grp", "sp"), "tp"),
        P("tp", None),
        P(),
        P("sp", "tp"),
        P("sp", "tp"),
        P("tp", "sp"),
    )
    out_specs = P(("grp", "sp", "tp"), None)
    return jax.shard_map(body, mesh=mesh, in_specs=in_specs, out_specs=out_specs, check_vma=False)
```

```python
import functools

import jax
import jax.numpy as jnp
from jax import lax
from jax.experimental import pallas as pl
from jax.experimental.pallas import tpu as pltpu
from jax.sharding import PartitionSpec as P

GATE_ROWS = 16
MASKED = -1e30


def swap_cores(value):
    n = lax.axis_size("sp")
    return lax.ppermute(value, "sp", [(i, i ^ 1) for i in range(n)])


def chip_shift(value, step):
    n = lax.axis_size("sp")
    return lax.ppermute(value, "sp", [(i, (i + 2 * step) % n) for i in range(n)])


def tp_shift(value, step):
    n = lax.axis_size("tp")
    return lax.ppermute(value, "tp", [(i, (i + step) % n) for i in range(n)])


def swap_groups(value):
    n = lax.axis_size("grp")
    return lax.ppermute(value, "grp", [(i, i ^ 1) for i in range(n)])


def three_parts(value):
    high = lax.reduce_precision(value, 8, 7)
    rest = value - high
    middle = lax.reduce_precision(rest, 8, 7)
    low = rest - middle
    return [p.astype(jnp.bfloat16) for p in (high, middle, low)]


def attend_block(heads, width, tile, qa_ref, key_read, value_read, top, total, opening):
    rows = qa_ref.shape[1]
    key_rows = heads * width
    tiles = rows // tile

    @pl.loop(0, heads * tiles)
    def _(step):
        h = step // tiles
        r = (step % tiles) * tile
        at = pl.ds(pl.multiple_of(r, tile), tile)
        lane = lax.broadcasted_iota(jnp.int32, (1, key_rows), 1)
        mine = (lane >= h * width) & (lane < (h + 1) * width)
        value_block = value_read()
        values = jnp.where(mine, value_block, jnp.ones_like(value_block))
        scores = jnp.dot(
            qa_ref[h, at, :], key_read(pl.ds(pl.multiple_of(h * width, width), width)),
            preferred_element_type=jnp.float32,
        )
        if opening:
            row = r + lax.broadcasted_iota(jnp.int32, scores.shape, 0)
            column = lax.broadcasted_iota(jnp.int32, scores.shape, 1)
            scores = jnp.where(row >= column, scores, MASKED)
        new_top = jnp.max(scores, axis=1, keepdims=True)
        if not opening:
            old_top = top[h, at, :1]
            new_top = jnp.maximum(old_top, new_top)
        weights = jnp.exp(scores - new_top).astype(jnp.bfloat16)
        product = jnp.dot(weights, values, preferred_element_type=jnp.float32)
        if not opening:
            product += total[h, at, :] * jnp.exp(old_top - new_top)
        total[h, at, :] = product
        top[h, at, :] = jnp.broadcast_to(new_top, (tile, top.shape[2]))


def reads(key_ref, value_ref, columns):
    value_start = value_ref.shape[0] - columns

    def key_read(rows):
        return jnp.concatenate([key_ref[rows, :], key_ref[columns : columns + GATE_ROWS, :]], axis=0)

    def value_read():
        blocks = range(0, value_ref.shape[1], columns)
        return jnp.concatenate([value_ref[value_start:, j : j + columns] for j in blocks], axis=0)

    return key_read, value_read


def attend_open_kernel(heads, width, tile, qa_ref, own_ref, top, total):
    read = reads(own_ref, own_ref, heads * width)
    attend_block(heads, width, tile, qa_ref, *read, top, total, True)


def attend_step_kernel(
    heads, width, tile, chips, k, place_ref, qa_ref, up_ref, down_ref, top_in, total_in, top, total
):
    place = place_ref[0]

    @pl.when(place - k >= 0)
    def _():
        read = reads(up_ref, up_ref, heads * width)
        attend_block(heads, width, tile, qa_ref, *read, top, total, False)

    @pl.when(place + k >= chips)
    def _():
        read = reads(down_ref, down_ref, heads * width)
        attend_block(heads, width, tile, qa_ref, *read, top, total, False)


def attend_last_kernel(
    heads, width, tile, k, place_ref, qa_ref, key_ref, value_ref, top_in, total_in, out_ref, top, total
):
    top[...] = top_in[...]
    total[...] = total_in[...]

    @pl.when(place_ref[0] - k >= 0)
    def _():
        read = reads(key_ref, value_ref, heads * width)
        attend_block(heads, width, tile, qa_ref, *read, top, total, False)

    lane = lax.broadcasted_iota(jnp.int32, (1, heads * width), 1)
    result = jnp.zeros(out_ref.shape, jnp.float32)
    for h in range(heads):
        sums = total[h, :, :]
        mine = (lane >= h * width) & (lane < (h + 1) * width)
        result = jnp.where(mine, sums / pltpu.roll(sums, width, 1), result)
    out_ref[...] = result.astype(out_ref.dtype)


TILE = 256


def attend_rings(heads, width, place, augmented, own, own_weights):
    chips = lax.axis_size("sp") // 2
    rows, keys = augmented.shape[1], own.shape[1]
    columns = heads * width
    local = pl.BlockSpec(memory_space=pltpu.VMEM)
    scalar = pl.BlockSpec(memory_space=pltpu.SMEM)
    state = [
        jax.ShapeDtypeStruct((heads, rows, 128), jnp.float32),
        jax.ShapeDtypeStruct((heads, rows, columns), jnp.float32),
    ]

    def cost(blocks):
        return pl.CostEstimate(
            flops=blocks * 4 * rows * keys * heads * 256,
            bytes_accessed=blocks * own.size * 2,
            transcendentals=blocks * rows * keys * heads,
        )

    params = pltpu.CompilerParams(vmem_limit_bytes=16 * 2**20)
    place = place.reshape(1)
    half = own_weights.shape[0] // 2
    side = lax.axis_index("grp") % 2
    w_up = w_down = jnp.where(side == 0, own_weights[:half], own_weights[half:])
    w_ups, w_downs, w_others = [], [], []
    up = down = own
    split = columns + GATE_ROWS
    top, total = pl.pallas_call(
        functools.partial(attend_open_kernel, heads, width, TILE),
        out_shape=state,
        in_specs=[local] * 2,
        out_specs=[local] * 2,
        compiler_params=params,
        cost_estimate=cost(1),
        name="attend_open",
    )(augmented, own)
    waits = {1: 0, 2: 1, 3: 3, 4: 4, 5: 6, 6: 8}
    arrived = [own]
    weight_step = 1

    def weights_forward(w_up, w_down, number):
        before = w_others[number - 3] if number > 2 else own_weights
        w_up, w_down, _, _ = lax.optimization_barrier((w_up, w_down, arrived[-1], before))
        if number == chips // 2:
            w_ups.append(chip_shift(w_up, 1))
            w_downs.append(chip_shift(w_others[-1][half:], -1))
            return w_up, w_down
        w_up, w_down = chip_shift(w_up, 1), chip_shift(w_down, -1)
        w_ups.append(w_up)
        w_downs.append(w_down)
        w_others.append(swap_groups(jnp.concatenate([w_up, w_down], axis=0)))
        return w_up, w_down

    for k in range(1, chips // 2 + 1):
        while weight_step < chips // 2 + 1 and waits.get(weight_step, chips) <= k - 1:
            w_up, w_down = weights_forward(w_up, w_down, weight_step)
            weight_step += 1
        if k < chips // 2:
            up, down = lax.optimization_barrier((chip_shift(up, 1), chip_shift(down, -1)))
            arrived.append(up)
            top, total = pl.pallas_call(
                functools.partial(attend_step_kernel, heads, width, TILE, chips, k),
                out_shape=state,
                in_specs=[scalar] + [local] * 5,
                out_specs=[local] * 2,
                input_output_aliases={4: 0, 5: 1},
                compiler_params=params,
                cost_estimate=cost(2),
                name="attend_step",
            )(place, augmented, up, down, top, total)
        else:
            first, second = chip_shift(up[:split], 1), chip_shift(down[split:], -1)
            arrived.append(first)
            attended = pl.pallas_call(
                functools.partial(attend_last_kernel, heads, width, TILE, k),
                out_shape=jax.ShapeDtypeStruct((rows, columns), jnp.bfloat16),
                in_specs=[scalar] + [local] * 5,
                out_specs=local,
                scratch_shapes=[pltpu.VMEM(s.shape, s.dtype) for s in state],
                compiler_params=params,
                cost_estimate=cost(1),
                name="attend_last",
            )(place, augmented, first, second, top, total)
    while weight_step <= chips // 2:
        w_up, w_down = weights_forward(w_up, w_down, weight_step)
        weight_step += 1
    near = chips // 2 - 1
    pieces = [own_weights] + w_ups[:near] + w_downs[:near] + w_others + [w_ups[-1], w_downs[-1]]
    return attended, pieces


def attend(queries, keys, values, log_gates, own_weights):
    rows = queries.shape[0]
    heads = log_gates.shape[1] // 2
    columns = queries.shape[1] // 2
    width = columns // heads
    chips = lax.axis_size("sp") // 2
    place = lax.axis_index("sp")
    core = place % 2
    gate_parts = jnp.concatenate(three_parts(log_gates), axis=1)
    gate_parts = gate_parts.reshape(rows, 3, 2, heads)
    sliced = [jnp.moveaxis(gate_parts, 2, 0).reshape(2, rows, 3 * heads)]
    packed = jnp.concatenate([queries, keys, values], axis=1).reshape(rows, 3, 2, columns)
    packed = jnp.moveaxis(packed, 2, 0).reshape(2, rows, 3 * columns)
    padding = jnp.zeros((2, rows, 128 - 3 * heads), jnp.bfloat16)
    packed = jnp.concatenate([packed, sliced[0], padding], axis=2)
    mine = jnp.where(core == 0, packed[0], packed[1])
    theirs = swap_cores(jnp.where(core == 0, packed[1], packed[0]))
    both = jnp.concatenate(
        [jnp.where(core == 0, mine, theirs), jnp.where(core == 0, theirs, mine)], axis=0
    )
    q, k, v = (both[:, i * columns : (i + 1) * columns] for i in range(3))
    gates = both[:, 3 * columns : 3 * columns + 3 * heads].reshape(2 * rows, 3, heads)
    scaled = (q.astype(jnp.float32) * (width**-0.5)).astype(jnp.bfloat16)
    one = jnp.ones((2 * rows, 3), jnp.bfloat16)
    zero = jnp.zeros((2 * rows, 3), jnp.bfloat16)
    augmented = []
    for h in range(heads):
        parts = [scaled[:, h * width : (h + 1) * width], gates[:, :, h]]
        parts += [one if g == h else zero for g in range(heads)]
        parts.append(jnp.zeros((2 * rows, GATE_ROWS - 3 - 3 * heads), jnp.bfloat16))
        augmented.append(jnp.concatenate(parts, axis=1))
    augmented = jnp.stack(augmented)
    gate_rows = jnp.concatenate(
        [one] + [-gates[:, :, h] for h in range(heads)]
        + [jnp.zeros((2 * rows, GATE_ROWS - 3 - 3 * heads), jnp.bfloat16)],
        axis=1,
    ).T
    value_rows = jnp.concatenate(
        [v[r : r + columns] for r in range(0, 2 * rows, columns)], axis=1
    )
    own = jnp.concatenate([k.T, gate_rows, value_rows], axis=0)
    return attend_rings(heads, width, place // 2, augmented, own, own_weights)


def in_core_order(mine, theirs, axis):
    core = lax.axis_index("sp") % 2
    first, second = jnp.where(core == 0, mine, theirs), jnp.where(core == 0, theirs, mine)
    return jnp.concatenate([first, second], axis=axis)


def project_kernel(groups, cols, place_ref, mine_ref, theirs_ref, *refs):
    weights, (own_ref, other_ref, gain_ref, mixed_ref, normed_ref) = refs[:groups], refs[groups:]
    core = place_ref[0] % 2
    rows, width = mine_ref.shape[0], mine_ref.shape[1] // groups
    half = rows // 2
    features = mixed_ref.shape[1]
    group = []
    for s in range(groups):
        mine = mine_ref[:, s * width : (s + 1) * width]
        theirs = theirs_ref[:, s * width : (s + 1) * width]
        first, second = jnp.where(core == 0, mine, theirs), jnp.where(core == 0, theirs, mine)
        group.append(jnp.concatenate([first, second], axis=1))
    squares = jnp.zeros((rows, 128), jnp.float32)
    for c in range(0, features, cols):
        at = slice(c, c + cols)
        projected = jnp.zeros((rows, cols), jnp.float32)
        for s in range(groups):
            product = jnp.dot(group[s], weights[s][:, at], preferred_element_type=jnp.float32)
            projected += product.astype(jnp.bfloat16).astype(jnp.float32)
        own, other = own_ref[:, at], other_ref[:, at]
        first, second = jnp.where(core == 0, own, other), jnp.where(core == 0, other, own)
        residual = jnp.concatenate([first, second], axis=0).astype(jnp.float32)
        mixed = (residual + projected).astype(jnp.bfloat16)
        mixed_ref[:, at] = mixed
        floats = mixed.astype(jnp.float32)
        for d in range(0, cols, 128):
            squares += floats[:, d : d + 128] * floats[:, d : d + 128]
    scale = lax.rsqrt(jnp.sum(squares, axis=1, keepdims=True) / features + 1e-06)
    for c in range(0, features, cols):
        at = slice(c, c + cols)
        normed = mixed_ref[:, at].astype(jnp.float32) * scale * gain_ref[:, at]
        normed_ref[:, at] = normed.astype(jnp.bfloat16)


def project(mine, theirs, weights, own, other, gain):
    rows, features = 2 * own.shape[0], own.shape[1]
    local = pl.BlockSpec(memory_space=pltpu.VMEM)
    place = lax.axis_index("sp")
    return pl.pallas_call(
        functools.partial(project_kernel, len(weights), 256),
        out_shape=[jax.ShapeDtypeStruct((rows, features), jnp.bfloat16)] * 2,
        in_specs=[pl.BlockSpec(memory_space=pltpu.SMEM)] + [local] * (5 + len(weights)),
        out_specs=[local] * 2,
        compiler_params=pltpu.CompilerParams(vmem_limit_bytes=40 * 2**20),
        cost_estimate=pl.CostEstimate(
            flops=2 * rows * features * 2 * mine.shape[1],
            bytes_accessed=2 * (3 * rows * features + 2 * mine.size),
            transcendentals=rows,
        ),
        name="project",
    )(place.reshape(1), mine, theirs, *weights, own, other, gain.reshape(1, features))


def feed_kernel(chips, cols, where_ref, normed_ref, *refs):
    near = chips // 2 - 1
    pieces, (kept_ref, sent_ref, held, sems) = refs[: 3 + 3 * near], refs[3 + 3 * near :]
    place, side = where_ref[0] // 2, where_ref[1]
    core = where_ref[0] % 2
    half = held.shape[0] // 2
    units = held.shape[0] // 3
    own, ups, downs = pieces[0], pieces[1 : 1 + near], pieces[1 + near : 1 + 2 * near]
    others, last = pieces[1 + 2 * near : 1 + 3 * near], pieces[1 + 3 * near :]

    def spot(chip, part):
        row = pl.multiple_of(part * half, 16)
        column = pl.multiple_of(lax.rem(chip + chips, chips) * 128, 128)
        return held.at[pl.ds(row, half), pl.ds(column, 128)]

    moves = [(own.at[pl.ds(0, half)], spot(place, 0)), (own.at[pl.ds(half, half)], spot(place, 1))]
    for k in range(1, near + 1):
        moves.append((ups[k - 1], spot(place - k, side)))
        moves.append((downs[k - 1], spot(place + k, side)))
        moves.append((others[k - 1].at[pl.ds(0, half)], spot(place - k, 1 - side)))
        moves.append((others[k - 1].at[pl.ds(half, half)], spot(place + k, 1 - side)))
    moves.append((last[0], spot(place + near + 1, side)))
    moves.append((last[1], spot(place + near + 1, 1 - side)))
    copies = [
        pltpu.make_async_copy(source, target, sems.at[i])
        for i, (source, target) in enumerate(moves)
    ]
    for copy in copies:
        copy.start()
    for copy in copies:
        copy.wait()
    contract = (((1,), (1,)), ((), ()))
    gate = lax.dot_general(
        normed_ref[...], held[:units, :], contract, preferred_element_type=jnp.float32
    )
    up = lax.dot_general(
        normed_ref[...], held[units : 2 * units, :], contract, preferred_element_type=jnp.float32
    )
    hidden = (gate / (1.0 + jnp.exp(-gate)) * up).astype(jnp.bfloat16)
    rows = hidden.shape[0] // 2
    for c in range(0, held.shape[1], cols):
        at = slice(c, c + cols)
        partial = jnp.dot(
            hidden, held[2 * units : 3 * units, at], preferred_element_type=jnp.float32
        )
        first, second = partial[:rows], partial[rows:]
        kept_ref[:, at] = jnp.where(core == 0, first, second)
        sent_ref[:, at] = jnp.where(core == 0, second, first).astype(jnp.bfloat16)


def feed(normed, pieces):
    chips = lax.axis_size("sp") // 2
    rows, features = normed.shape
    anywhere = pl.BlockSpec(memory_space=pl.ANY)
    local = pl.BlockSpec(memory_space=pltpu.VMEM)
    where = jnp.stack([lax.axis_index("sp"), lax.axis_index("grp") % 2])
    depth = pieces[0].shape[0]
    return pl.pallas_call(
        functools.partial(feed_kernel, chips, 512),
        out_shape=[
            jax.ShapeDtypeStruct((rows // 2, features), jnp.float32),
            jax.ShapeDtypeStruct((rows // 2, features), jnp.bfloat16),
        ],
        in_specs=[pl.BlockSpec(memory_space=pltpu.SMEM), local] + [anywhere] * len(pieces),
        out_specs=[local] * 2,
        scratch_shapes=[
            pltpu.VMEM((depth, features), jnp.bfloat16),
            pltpu.SemaphoreType.DMA((2 * chips,)),
        ],
        compiler_params=pltpu.CompilerParams(vmem_limit_bytes=48 * 2**20),
        cost_estimate=pl.CostEstimate(
            flops=2 * rows * features * depth,
            bytes_accessed=2 * (depth * features + 2 * rows * features),
            transcendentals=rows * depth // 3,
        ),
        name="feed",
    )(where, normed, *pieces)


def body(residual, queries, keys, values, log_gates, w_out, norm_gain, w_gate, w_up, w_down):
    tp = lax.axis_size("tp")
    core = lax.axis_index("sp") % 2
    units = w_down.shape[0] // 2
    shard = jnp.stack([w_gate.T, w_up.T, w_down]).reshape(3, 2, units, -1)
    shard = jnp.moveaxis(shard, 1, 0).reshape(2, 3 * units, -1)
    mine = jnp.where(core == 0, shard[0], shard[1])
    theirs = swap_cores(jnp.where(core == 0, shard[1], shard[0]))
    own_weights = in_core_order(mine, theirs, 1)
    other_residual = swap_cores(residual)
    out_weights = [w_out] + [tp_shift(w_out, s) for s in range(1, tp)]
    attended, pieces = attend(queries, keys, values, log_gates, own_weights)
    groups = [attended] + [tp_shift(attended, s) for s in range(1, tp)]
    mine = jnp.concatenate(groups, axis=1)
    mixed, normed = project(
        mine, swap_cores(mine), out_weights, residual, other_residual, norm_gain
    )
    kept, sent = feed(normed, pieces)
    partial = (kept + swap_cores(sent).astype(jnp.float32)).astype(jnp.bfloat16)
    per_device = partial.shape[0] // tp
    place = lax.axis_index("tp")

    def rows_of(value, index):
        return lax.dynamic_slice_in_dim(value, index * per_device, per_device, 0)

    down_sum = rows_of(partial, place).astype(jnp.float32)
    for s in range(1, tp):
        down_sum += tp_shift(rows_of(partial, (place + s) % tp), s).astype(jnp.float32)
    summed = rows_of(mixed, core * tp + place).astype(jnp.float32) + 0.5 * down_sum
    scaled = summed * lax.rsqrt(jnp.mean(summed * summed, axis=-1, keepdims=True) + 1e-06)
    return scaled.astype(jnp.bfloat16)


def solution(mesh):
    in_specs = (
        P(("grp", "sp"), None),
        P(("grp", "sp"), "tp"),
        P(("grp", "sp"), "tp"),
        P(("grp", "sp"), "tp"),
        P(("grp", "sp"), "tp"),
        P("tp", None),
        P(),
        P("sp", "tp"),
        P("sp", "tp"),
        P("tp", "sp"),
    )
    out_specs = P(("grp", "sp", "tp"), None)
    return jax.shard_map(body, mesh=mesh, in_specs=in_specs, out_specs=out_specs, check_vma=False)
```

```python
import functools

import jax
import jax.numpy as jnp
from jax import lax
from jax.experimental import pallas as pl
from jax.experimental.pallas import tpu as pltpu
from jax.sharding import PartitionSpec as P

GATE_ROWS = 16
MASKED = -1e30


def swap_cores(value):
    n = lax.axis_size("sp")
    return lax.ppermute(value, "sp", [(i, i ^ 1) for i in range(n)])


def chip_shift(value, step):
    n = lax.axis_size("sp")
    return lax.ppermute(value, "sp", [(i, (i + 2 * step) % n) for i in range(n)])


def tp_shift(value, step):
    n = lax.axis_size("tp")
    return lax.ppermute(value, "tp", [(i, (i + step) % n) for i in range(n)])


def swap_groups(value):
    n = lax.axis_size("grp")
    return lax.ppermute(value, "grp", [(i, i ^ 1) for i in range(n)])


def prepare_rows_kernel(heads, width, place_ref, q_ref, k_ref, v_ref, gates_ref, mine_ref, theirs_ref):
    core = place_ref[0] % 2
    columns = heads * width
    rows = q_ref.shape[0]
    gates = gates_ref[...]
    line = lax.broadcasted_iota(jnp.int32, (GATE_ROWS, rows), 0)
    for out_ref, half in ((mine_ref, core), (theirs_ref, 1 - core)):
        at = pl.ds(pl.multiple_of(half * columns, columns), columns)
        k = k_ref[:, at]
        for j in range(rows // columns):
            out_ref[:columns, j * columns : (j + 1) * columns] = k[j * columns : (j + 1) * columns]
        block = jnp.where(line < 3, 1.0, 0.0)
        for h in range(heads):
            value = jnp.where(half == 0, gates[h : h + 1], gates[heads + h : heads + h + 1])
            for p in range(3):
                part = value.astype(jnp.bfloat16).astype(jnp.float32)
                block = jnp.where(line == 3 + 3 * h + p, -part, block)
                value = value - part
        out_ref[columns : columns + GATE_ROWS, :] = block.astype(jnp.bfloat16)
        start = columns + GATE_ROWS
        v = v_ref[:, at].astype(jnp.float32)
        out_ref[start : start + columns, :] = v.T.astype(jnp.bfloat16)
        q = q_ref[:, at].astype(jnp.float32) * (width**-0.5)
        out_ref[start + columns : start + 2 * columns, :] = q.T.astype(jnp.bfloat16)


def prepare_weights_kernel(place_ref, gate_ref, up_ref, down_ref, mine_ref, theirs_ref):
    core = place_ref[0] % 2
    units = down_ref.shape[0] // 2
    gate = gate_ref[...].astype(jnp.float32).T.astype(jnp.bfloat16)
    up = up_ref[...].astype(jnp.float32).T.astype(jnp.bfloat16)
    for i, value in enumerate((gate, up, down_ref[...])):
        first, second = value[:units], value[units:]
        at = slice(i * units, (i + 1) * units)
        mine_ref[at, :] = jnp.where(core == 0, first, second)
        theirs_ref[at, :] = jnp.where(core == 0, second, first)


def attend_kernel(chips, heads, width, place_ref, chip_ref, *refs):
    whole = chips - 2
    pieces, rest = refs[:whole], refs[whole:]
    first_ref, second_ref, out_ref, held, query, top, total = rest
    place = place_ref[0]
    columns = heads * width
    split = columns + GATE_ROWS
    depth = split + columns
    rows = chip_ref.shape[1]
    cut = rows // 2
    line = lax.broadcasted_iota(jnp.int32, (GATE_ROWS, rows), 0)
    feature = lax.broadcasted_iota(jnp.int32, (columns, rows), 0)
    own_gates = chip_ref[columns:split, :].astype(jnp.float32)
    own_queries = chip_ref[depth : depth + columns, :]
    for h in range(heads):
        mine = (feature >= h * width) & (feature < (h + 1) * width)
        query[h, :columns, :] = jnp.where(mine, own_queries, jnp.zeros_like(own_queries))
        block = jnp.where((line >= 3 + 3 * h) & (line < 6 + 3 * h), 1.0, 0.0)
        for p in range(3):
            block = jnp.where(line == p, -own_gates[3 + 3 * h + p : 4 + 3 * h + p], block)
        query[h, columns:split, :] = block.astype(jnp.bfloat16)

    def block(read, opening):
        keys = jnp.concatenate([read(0, columns, j, columns) for j in range(0, rows, columns)], axis=0)
        gates = read(columns, GATE_ROWS, 0, rows).astype(jnp.float32).T.astype(jnp.bfloat16)
        keys = jnp.concatenate([keys, gates], axis=1)
        values = [
            jnp.concatenate(
                [read(split + h * width, width, 0, rows), jnp.ones((GATE_ROWS, rows), jnp.bfloat16)],
                axis=0,
            )
            for h in range(heads)
        ]
        parts = [(h, c) for h in range(heads) for c in range(0, rows, cut)]

        def scored(h, c):
            scores = jnp.dot(
                keys, query[h, :, c : c + cut], preferred_element_type=jnp.float32
            )
            if opening:
                key = lax.broadcasted_iota(jnp.int32, scores.shape, 0)
                asked = c + lax.broadcasted_iota(jnp.int32, scores.shape, 1)
                scores = jnp.where(asked >= key, scores, MASKED)
            return scores

        upcoming = scored(*parts[0])
        for i, (h, c) in enumerate(parts):
            scores = upcoming
            if i + 1 < len(parts):
                upcoming = scored(*parts[i + 1])
            at = slice(c, c + cut)
            new_top = jnp.max(scores, axis=0, keepdims=True)
            if not opening:
                old_top = top[h, :1, at]
                new_top = jnp.maximum(old_top, new_top)
            weights = jnp.exp(scores - new_top).astype(jnp.bfloat16)
            product = jnp.dot(values[h], weights, preferred_element_type=jnp.float32)
            if not opening:
                product += total[h, :, at] * jnp.exp(old_top - new_top)
            total[h, :, at] = product
            top[h, :1, at] = new_top

    block(lambda r, m, c, n: chip_ref[r : r + m, c : c + n], True)
    half = chips // 2

    def excess(i):
        return jnp.where(
            i < half - 1,
            place - (i + 1),
            jnp.where(i < whole, place + (i - half + 2) - chips, place - half),
        )

    for i, piece in enumerate(pieces):

        @pl.when(excess(i) >= 0)
        def _():
            held[i] = piece[...]

    @pl.when(excess(whole) >= 0)
    def _():
        held[whole, :split] = first_ref[...]
        held[whole, split:] = second_ref[...]

    @pl.loop(0, chips - 1)
    def _(i):
        @pl.when(excess(i) >= 0)
        def _():
            block(lambda r, m, c, n: held[i, r : r + m, c : c + n], False)

    result = jnp.concatenate(
        [total[h, :width, :] / total[h, width : width + 1, :] for h in range(heads)], axis=0
    )
    out_ref[...] = result.T.astype(out_ref.dtype)


def attend_call(heads, width, place, chip, pieces, halves):
    chips = lax.axis_size("sp") // 2
    rows, columns = chip.shape[1], heads * width
    split = columns + GATE_ROWS
    local = pl.BlockSpec(memory_space=pltpu.VMEM)
    return pl.pallas_call(
        functools.partial(attend_kernel, chips, heads, width),
        out_shape=jax.ShapeDtypeStruct((rows, columns), jnp.bfloat16),
        in_specs=[pl.BlockSpec(memory_space=pltpu.SMEM), local] + [local] * chips,
        out_specs=local,
        scratch_shapes=[
            pltpu.VMEM((chips - 1, split + columns, rows), jnp.bfloat16),
            pltpu.VMEM((heads, split, rows), jnp.bfloat16),
            pltpu.VMEM((heads, 8, rows), jnp.float32),
            pltpu.VMEM((heads, width + GATE_ROWS, rows), jnp.float32),
        ],
        compiler_params=pltpu.CompilerParams(vmem_limit_bytes=16 * 2**20),
        cost_estimate=pl.CostEstimate(
            flops=chips * 4 * rows * rows * heads * 256,
            bytes_accessed=chips * (split + columns) * rows * 2,
            transcendentals=chips * rows * rows * heads,
        ),
        name="attend",
    )(place, chip, *pieces, *halves)


def rings(own, own_weights):
    chips = lax.axis_size("sp") // 2
    half = own_weights.shape[0] // 2
    side = lax.axis_index("grp") % 2
    w_up = w_down = jnp.where(side == 0, own_weights[:half], own_weights[half:])
    w_ups, w_downs, w_others = [], [], []
    up = down = own
    split = own.shape[0] // 2 + GATE_ROWS // 2
    ups, downs = [], []
    waits = {1: 0, 2: 1, 3: 3, 4: 4, 5: 6, 6: 8}
    arrived = [own]
    weight_step = 1

    def weights_forward(w_up, w_down, number):
        before = w_others[number - 3] if number > 2 else own_weights
        w_up, w_down, _, _ = lax.optimization_barrier((w_up, w_down, arrived[-1], before))
        if number == chips // 2:
            w_ups.append(chip_shift(w_up, 1))
            w_downs.append(chip_shift(w_others[-1][half:], -1))
            return w_up, w_down
        w_up, w_down = chip_shift(w_up, 1), chip_shift(w_down, -1)
        w_ups.append(w_up)
        w_downs.append(w_down)
        w_others.append(swap_groups(jnp.concatenate([w_up, w_down], axis=0)))
        return w_up, w_down

    for k in range(1, chips // 2 + 1):
        while weight_step < chips // 2 + 1 and waits.get(weight_step, chips) <= k - 1:
            w_up, w_down = weights_forward(w_up, w_down, weight_step)
            weight_step += 1
        if k < chips // 2:
            up, down = lax.optimization_barrier((chip_shift(up, 1), chip_shift(down, -1)))
            ups.append(up)
            downs.append(down)
            arrived.append(up)
        else:
            halves = (chip_shift(up[:split], 1), chip_shift(down[split:], -1))
            arrived.append(halves[0])
    while weight_step <= chips // 2:
        w_up, w_down = weights_forward(w_up, w_down, weight_step)
        weight_step += 1
    near = chips // 2 - 1
    weights = [own_weights] + w_ups[:near] + w_downs[:near] + w_others + [w_ups[-1], w_downs[-1]]
    return ups + downs, halves, weights


def prepare(queries, keys, values, log_gates, w_gate, w_up, w_down):
    rows = queries.shape[0]
    heads = log_gates.shape[1] // 2
    columns = queries.shape[1] // 2
    width = columns // heads
    place = lax.axis_index("sp").reshape(1)
    local = pl.BlockSpec(memory_space=pltpu.VMEM)
    scalar = pl.BlockSpec(memory_space=pltpu.SMEM)
    packed = jax.ShapeDtypeStruct((3 * columns + GATE_ROWS, rows), jnp.bfloat16)
    mine, theirs = pl.pallas_call(
        functools.partial(prepare_rows_kernel, heads, width),
        out_shape=[packed] * 2,
        in_specs=[scalar] + [local] * 4,
        out_specs=[local] * 2,
        name="prepare_rows",
    )(place, queries, keys, values, log_gates.T)
    chip = in_core_order(mine, swap_cores(theirs), 1)
    shard = jax.ShapeDtypeStruct((3 * w_down.shape[0] // 2, w_down.shape[1]), jnp.bfloat16)
    mine, theirs = pl.pallas_call(
        prepare_weights_kernel,
        out_shape=[shard] * 2,
        in_specs=[scalar] + [local] * 3,
        out_specs=[local] * 2,
        name="prepare_weights",
    )(place, w_gate, w_up, w_down)
    return chip, in_core_order(mine, swap_cores(theirs), 1), heads, width


def in_core_order(mine, theirs, axis):
    core = lax.axis_index("sp") % 2
    first, second = jnp.where(core == 0, mine, theirs), jnp.where(core == 0, theirs, mine)
    return jnp.concatenate([first, second], axis=axis)


def project_kernel(groups, cols, place_ref, mine_ref, theirs_ref, *refs):
    weights, (own_ref, other_ref, gain_ref, mixed_ref, normed_ref) = refs[:groups], refs[groups:]
    core = place_ref[0] % 2
    rows, width = mine_ref.shape[0], mine_ref.shape[1] // groups
    half = rows // 2
    features = mixed_ref.shape[1]
    group = []
    for s in range(groups):
        mine = mine_ref[:, s * width : (s + 1) * width]
        theirs = theirs_ref[:, s * width : (s + 1) * width]
        first, second = jnp.where(core == 0, mine, theirs), jnp.where(core == 0, theirs, mine)
        group.append(jnp.concatenate([first, second], axis=1))
    squares = jnp.zeros((rows, 128), jnp.float32)
    for c in range(0, features, cols):
        at = slice(c, c + cols)
        projected = jnp.zeros((rows, cols), jnp.float32)
        for s in range(groups):
            product = jnp.dot(group[s], weights[s][:, at], preferred_element_type=jnp.float32)
            projected += product.astype(jnp.bfloat16).astype(jnp.float32)
        own, other = own_ref[:, at], other_ref[:, at]
        first, second = jnp.where(core == 0, own, other), jnp.where(core == 0, other, own)
        residual = jnp.concatenate([first, second], axis=0).astype(jnp.float32)
        mixed = (residual + projected).astype(jnp.bfloat16)
        mixed_ref[:, at] = mixed
        floats = mixed.astype(jnp.float32)
        for d in range(0, cols, 128):
            squares += floats[:, d : d + 128] * floats[:, d : d + 128]
    scale = lax.rsqrt(jnp.sum(squares, axis=1, keepdims=True) / features + 1e-06)
    for c in range(0, features, cols):
        at = slice(c, c + cols)
        normed = mixed_ref[:, at].astype(jnp.float32) * scale * gain_ref[:, at]
        normed_ref[:, at] = normed.astype(jnp.bfloat16)


def project(mine, theirs, weights, own, other, gain):
    rows, features = 2 * own.shape[0], own.shape[1]
    local = pl.BlockSpec(memory_space=pltpu.VMEM)
    place = lax.axis_index("sp")
    return pl.pallas_call(
        functools.partial(project_kernel, len(weights), 256),
        out_shape=[jax.ShapeDtypeStruct((rows, features), jnp.bfloat16)] * 2,
        in_specs=[pl.BlockSpec(memory_space=pltpu.SMEM)] + [local] * (5 + len(weights)),
        out_specs=[local] * 2,
        compiler_params=pltpu.CompilerParams(vmem_limit_bytes=16 * 2**20),
        cost_estimate=pl.CostEstimate(
            flops=2 * rows * features * 2 * mine.shape[1],
            bytes_accessed=2 * (3 * rows * features + 2 * mine.size),
            transcendentals=rows,
        ),
        name="project",
    )(place.reshape(1), mine, theirs, *weights, own, other, gain.reshape(1, features))


def feed_kernel(chips, cols, where_ref, normed_ref, *refs):
    near = chips // 2 - 1
    pieces, (kept_ref, sent_ref, held) = refs[: 3 + 3 * near], refs[3 + 3 * near :]
    place, side = where_ref[0] // 2, where_ref[1]
    core = where_ref[0] % 2
    half = held.shape[0] // 2
    units = held.shape[0] // 3
    own, ups, downs = pieces[0], pieces[1 : 1 + near], pieces[1 + near : 1 + 2 * near]
    others, last = pieces[1 + 2 * near : 1 + 3 * near], pieces[1 + 3 * near :]

    def put(chip, part, value):
        row = pl.multiple_of(part * half, 16)
        column = pl.multiple_of(lax.rem(chip + chips, chips) * 128, 128)
        held[pl.ds(row, half), pl.ds(column, 128)] = value

    put(place, 0, own[:half, :])
    put(place, 1, own[half:, :])
    for k in range(1, near + 1):
        put(place - k, side, ups[k - 1][...])
        put(place + k, side, downs[k - 1][...])
        put(place - k, 1 - side, others[k - 1][:half, :])
        put(place + k, 1 - side, others[k - 1][half:, :])
    put(place + near + 1, side, last[0][...])
    put(place + near + 1, 1 - side, last[1][...])
    contract = (((1,), (1,)), ((), ()))
    gate = lax.dot_general(
        normed_ref[...], held[:units, :], contract, preferred_element_type=jnp.float32
    )
    up = lax.dot_general(
        normed_ref[...], held[units : 2 * units, :], contract, preferred_element_type=jnp.float32
    )
    hidden = (gate / (1.0 + jnp.exp(-gate)) * up).astype(jnp.bfloat16)
    rows = hidden.shape[0] // 2
    for c in range(0, held.shape[1], cols):
        at = slice(c, c + cols)
        partial = jnp.dot(
            hidden, held[2 * units : 3 * units, at], preferred_element_type=jnp.float32
        )
        first, second = partial[:rows], partial[rows:]
        kept_ref[:, at] = jnp.where(core == 0, first, second)
        sent_ref[:, at] = jnp.where(core == 0, second, first).astype(jnp.bfloat16)


def feed(normed, pieces):
    chips = lax.axis_size("sp") // 2
    rows, features = normed.shape
    local = pl.BlockSpec(memory_space=pltpu.VMEM)
    where = jnp.stack([lax.axis_index("sp"), lax.axis_index("grp") % 2])
    depth = pieces[0].shape[0]
    return pl.pallas_call(
        functools.partial(feed_kernel, chips, 512),
        out_shape=[
            jax.ShapeDtypeStruct((rows // 2, features), jnp.float32),
            jax.ShapeDtypeStruct((rows // 2, features), jnp.bfloat16),
        ],
        in_specs=[pl.BlockSpec(memory_space=pltpu.SMEM), local] + [local] * len(pieces),
        out_specs=[local] * 2,
        scratch_shapes=[
            pltpu.VMEM((depth, features), jnp.bfloat16),
        ],
        compiler_params=pltpu.CompilerParams(vmem_limit_bytes=24 * 2**20),
        cost_estimate=pl.CostEstimate(
            flops=2 * rows * features * depth,
            bytes_accessed=2 * (depth * features + 2 * rows * features),
            transcendentals=rows * depth // 3,
        ),
        name="feed",
    )(where, normed, *pieces)


def body(residual, queries, keys, values, log_gates, w_out, norm_gain, w_gate, w_up, w_down):
    tp = lax.axis_size("tp")
    core = lax.axis_index("sp") % 2
    chip, own_weights, heads, width = prepare(
        queries, keys, values, log_gates, w_gate, w_up, w_down
    )
    kept = chip.shape[0] - heads * width
    pieces, halves, weights = rings(chip[:kept], own_weights)
    other_residual = swap_cores(residual)
    out_weights = [w_out] + [tp_shift(w_out, s) for s in range(1, tp)]
    place = (lax.axis_index("sp") // 2).reshape(1)
    attended = attend_call(heads, width, place, chip, pieces, halves)
    groups = [attended] + [tp_shift(attended, s) for s in range(1, tp)]
    mine = jnp.concatenate(groups, axis=1)
    mixed, normed = project(
        mine, swap_cores(mine), out_weights, residual, other_residual, norm_gain
    )
    kept, sent = feed(normed, weights)
    partial = (kept + swap_cores(sent).astype(jnp.float32)).astype(jnp.bfloat16)
    per_device = partial.shape[0] // tp
    place = lax.axis_index("tp")

    def rows_of(value, index):
        return lax.dynamic_slice_in_dim(value, index * per_device, per_device, 0)

    down_sum = rows_of(partial, place).astype(jnp.float32)
    for s in range(1, tp):
        down_sum += tp_shift(rows_of(partial, (place + s) % tp), s).astype(jnp.float32)
    summed = rows_of(mixed, core * tp + place).astype(jnp.float32) + 0.5 * down_sum
    scaled = summed * lax.rsqrt(jnp.mean(summed * summed, axis=-1, keepdims=True) + 1e-06)
    return scaled.astype(jnp.bfloat16)


def solution(mesh):
    in_specs = (
        P(("grp", "sp"), None),
        P(("grp", "sp"), "tp"),
        P(("grp", "sp"), "tp"),
        P(("grp", "sp"), "tp"),
        P(("grp", "sp"), "tp"),
        P("tp", None),
        P(),
        P("sp", "tp"),
        P("sp", "tp"),
        P("tp", "sp"),
    )
    out_specs = P(("grp", "sp", "tp"), None)
    return jax.shard_map(body, mesh=mesh, in_specs=in_specs, out_specs=out_specs, check_vma=False)
```
